32 devices in a mesh: sp: 8 (over z, x), tp: 4 (over y, core).
Axes of the slice: x: 2, y: 2, z: 4, core: 2. Of those that a mesh axis runs over, the one named last changes fastest.
Arguments:
- residual: bfloat16 [1536, 2048], P('sp', 'tp'), may hold values from -10 to 10
- queries: bfloat16 [1536, 16, 128], P('sp', 'tp'), may hold values from -6.5 to 6.5
- key_rows: bfloat16 [1536, 16, 128], P('sp', 'tp'), may hold values from -6.5 to 6.5
- value_rows: bfloat16 [1536, 16, 128], P('sp', 'tp'), may hold values from -6 to 6
- diff_scale: float32 [16], P('tp'), may hold values from 0.3 to 0.8
- head_gain: float32 [128], replicated, may hold values from 0.1 to 1.9
- out_weight: bfloat16 [2048, 2048], P(None, 'tp'), may hold values from -0.125 to 0.125
- norm_gain: float32 [2048], replicated, may hold values from 0.1 to 1.9
- gate_weight: bfloat16 [8, 2048, 4096], P('sp', None, 'tp'), may hold values from -0.5 to 0.5
- up_weight: bfloat16 [8, 2048, 4096], P('sp', None, 'tp'), may hold values from -0.5 to 0.5
- down_weight: bfloat16 [8, 4096, 2048], P('sp', None, 'tp'), may hold values from -0.01171875 to 0.01171875
- expert_ids: int32 [1536, 2], P('sp'), may hold values from 0 to 7, all different within a row; in each aligned block of 192 rows (0 to 191, 192 to 383, ...) at most 96 rows name the same one
- route_logit: float32 [1536, 2], P('sp'), may hold values from -6 to 6
Outputs:
- updated: bfloat16 [1536, 2048], P('sp', 'tp')
The draws below stay inside these ranges and needn't reach their ends.
Inputs may be any that keep to these rules, and one draw needn't show every extreme that they name: `expert_ids`: A token's 2 experts differ. The 192 tokens of one index of sp name one expert at most 96 times, a bound that some block reaches on some index.
All inputs are finite; a program needn't handle non-finite values.
Results may differ from the reference program's by a relative error of at most 0.014.
Values may be sent and summed in bfloat16 or wider, within the bound.
No kernel may reach another device: no remote copies, remote signals or barrier semaphores. Data moves between devices by JAX's collectives and lax.ppermute only.
A program may use at most 64 MiB of HBM per device.

```python
import math
import jax
import jax.numpy as jnp
import numpy as np
from jax import lax

D = 2048
HEADS = 16
QK = 64
V = 128
FF = 4096
TOP = 2
SPAN = 64
TOK_DEV = 192
TOKENS = 1536
EXPERTS = 8
CAP = 96
N_SP = 8


def drawn_pair(base):
    folded_key = jax.random.fold_in(base, 17)
    keys_list = jax.random.split(folded_key, 2)
    array_shape = (TOKENS, HEADS, 2 * QK)
    query_values = jnp.clip(1.3 * jax.random.normal(keys_list[0], array_shape, jnp.float32), -6.5, 6.5)
    key_values = jnp.clip(1.3 * jax.random.normal(keys_list[1], array_shape, jnp.float32), -6.5, 6.5)
    return (query_values, key_values)


def draw_queries(key, part):
    return drawn_pair(key)[0].astype(jnp.bfloat16)


def draw_key_rows(key, part):
    return drawn_pair(key)[1].astype(jnp.bfloat16)


def draw_residual(key, part):
    first = jax.random.fold_in(jax.random.fold_in(key, 29), 0)
    column = jnp.arange(D, dtype=jnp.float32) / D
    values = jnp.clip(jax.random.normal(first, (TOKENS, D), jnp.float32), -6.0, 6.0) * 0.5 * 3.0 ** column
    return values.astype(jnp.bfloat16)


def steps_of(rng, dims, cuts, least, top_value):
    factor_of, own = 1.0, jax.random.fold_in(rng, 6)
    for position, shards_of in cuts:
        steps = jnp.exp(jax.random.uniform(jax.random.fold_in(own, position), (shards_of,), jnp.float32, least / len(cuts), top_value / len(cuts)))
        factor_of = factor_of * jnp.repeat(steps, dims[position] // shards_of).reshape([-1 if axis == position else 1 for axis in range(len(dims))])
    return factor_of


def assign_block(rng, own, number, rows, number_of, top, limit, slope):
    sequence = jax.random.permutation(rng, number_of)
    packed, usual = portions_of(number_of, rows * top, limit, slope, True), portions_of(number_of, rows * top, limit, slope, False)
    places = jnp.arange(number_of)

    def named(tallies, offset_by):
        used = int((tallies > 0).sum())
        fixed = max(1, used // 4)
        passed = fixed + (places - fixed + offset_by * (used - fixed)) % max(1, number_of - fixed)
        return jnp.zeros((number_of,), jnp.int32).at[sequence[jnp.where(places < fixed, places, passed)]].set(jnp.asarray(tallies, jnp.int32))

    tallies = jnp.where(number % 4 == 0, named(packed, number // 4), named(usual, number - number // 4 - 1))
    mixed = jax.random.permutation(jax.random.fold_in(own, 3), number_of)
    donor, taker = mixed[0:number_of // 2 * 2:2], mixed[1:number_of // 2 * 2:2]
    margin = jnp.minimum(tallies[donor] - 1, limit - tallies[taker]) // 2
    margin = jnp.where((donor == sequence[0]) | (taker == sequence[0]) | (tallies[taker] == 0), 0, jnp.maximum(margin, 0))
    passed = jax.random.randint(jax.random.fold_in(own, 4), (number_of // 2,), 0, 1 << 20) % (margin + 1)
    tallies = tallies.at[donor].add(-passed).at[taker].add(passed)
    items = jnp.searchsorted(jnp.cumsum(tallies), jnp.arange(rows * top), side="right").astype(jnp.int32)
    listing = items.reshape(top, rows).T
    listing = listing[jax.random.permutation(jax.random.fold_in(own, 1), rows)]
    offset_by = jax.random.randint(jax.random.fold_in(own, 2), (rows, 1), 0, top)
    return jnp.take_along_axis(listing, (jnp.arange(top)[None, :] + offset_by) % top, axis=1)


def portions_of(number_of, total, reach, skew, full):
    portions = [(1 << 20) // math.isqrt(grade ** skew) + 1 for grade in range(1, number_of + 1)]
    largest = reach if full else min(reach, max(-(-total // number_of), total * portions[0] // sum(portions)))
    least = 1 if total - largest >= number_of - 1 else 0
    counts, rest = [largest] + [least] * (number_of - 1), total - largest - least * (number_of - 1)
    while rest > 0:
        free = [i for i in range(1, number_of) if counts[i] < largest] or [i for i in range(1, number_of) if counts[i] < reach]
        pool, remaining = sum([portions[i] for i in free]), rest
        for i in free:
            more = min(reach - counts[i], max(1, remaining * portions[i] // pool), rest)
            counts[i] = counts[i] + more
            rest = rest - more
    return np.array(counts)


def centred(own_key, extent, deviation, most, pieces=(), held_as=jnp.bfloat16):
    values = deviation * jax.random.normal(own_key, extent, jnp.float32)
    if pieces:
        values = values * steps_of(own_key, extent, pieces, -0.22, 0.18)
    return jnp.clip(values, -most, most).astype(held_as)


def setup_inputs(seed: int = 0) -> dict:
    keys = jax.random.split(jax.random.key(seed), 14)
    residual = draw_residual(jax.random.fold_in(keys[13], 71), 0)
    queries = draw_queries(jax.random.fold_in(keys[13], 71), 0)
    key_rows = draw_key_rows(jax.random.fold_in(keys[13], 71), 0)
    value_rows = centred(keys[3], (TOKENS, HEADS, V), 1.0, 6.0, ((0, 8), (1, 4)))
    diff_scale = jnp.clip(0.3 + 0.5 * jax.random.uniform(keys[4], (HEADS,), jnp.float32) ** steps_of(keys[4], (HEADS,), ((0, 4),), -0.2, 0.2), 0.3, 0.8)
    head_gain = jnp.clip(1.0 + 0.18 * jax.random.normal(keys[5], (V,), jnp.float32), 0.1, 1.9)
    out_weight = centred(keys[6], (HEADS * V, D), (HEADS * V) ** -0.5, 0.125, ((1, 4),))
    norm_gain = jnp.clip(1.0 + 0.18 * jax.random.normal(keys[7], (D,), jnp.float32), 0.1, 1.9)
    gate_weight = centred(keys[8], (EXPERTS, D, FF), (D // 16) ** -0.5, 0.5, ((0, 8), (2, 4)))
    up_weight = centred(keys[9], (EXPERTS, D, FF), (D // 16) ** -0.5, 0.5, ((0, 8), (2, 4)))
    down_weight = centred(keys[10], (EXPERTS, FF, D), (FF * 64) ** -0.5, 0.01171875, ((0, 8), (2, 4)))
    expert_ids_keys = jax.random.split(jax.random.fold_in(keys[11], 1), TOKENS // TOK_DEV)
    expert_ids_turns = jax.random.permutation(jax.random.fold_in(keys[11], 3), TOKENS // TOK_DEV)
    expert_ids = jax.vmap(lambda own, number: assign_block(jax.random.fold_in(keys[11], 2), own, number, TOK_DEV, EXPERTS, TOP, CAP, 2))(expert_ids_keys, expert_ids_turns).reshape((TOKENS, TOP))
    route_logit = centred(keys[12], (TOKENS, TOP), 1.5, 6.0, ((0, 8),), jnp.float32)
    return {"residual": residual, "queries": queries, "key_rows": key_rows, "value_rows": value_rows, "diff_scale": diff_scale, "head_gain": head_gain, "out_weight": out_weight, "norm_gain": norm_gain, "gate_weight": gate_weight, "up_weight": up_weight, "down_weight": down_weight, "expert_ids": expert_ids, "route_logit": route_logit}


NORM_EPS = 1e-05
CLAMP_LIMIT = 7.0
SWISH_ALPHA = 1.702
HEAD_KEEP = 0.8

def one_map(query_half, key_half, value_all, visible):
    scores = jnp.einsum('qhd,khd->hqk', query_half, key_half) * QK ** (-0.5)
    scores = jnp.where(visible[None], scores, -jnp.inf)
    row_peak = lax.optimization_barrier(jnp.max(scores, axis=-1, keepdims=True))
    exp_weights = jnp.where(visible[None], jnp.exp(scores - row_peak), 0.0)
    row_total = lax.optimization_barrier(jnp.sum(exp_weights, axis=-1))
    rounded = lax.optimization_barrier(exp_weights.astype(jnp.bfloat16)).astype(jnp.float32)
    accum = jnp.einsum('hqk,khv->hqv', rounded, value_all)
    return accum / row_total[..., None]

def reference(residual, queries, key_rows, value_rows, diff_scale, head_gain, out_weight, norm_gain, gate_weight, up_weight, down_weight, expert_ids, route_logit):
    block_rows = math.gcd(TOKENS, 512)
    key_all = key_rows.astype(jnp.float32)
    value_all = value_rows.astype(jnp.float32)
    key_span = jnp.arange(TOKENS, dtype=jnp.int32) // SPAN

    def attend(block_index):
        first_row = (block_index * block_rows).astype(jnp.int32)
        query_block = lax.dynamic_slice_in_dim(queries, first_row, block_rows, 0).astype(jnp.float32)
        query_span = (first_row + jnp.arange(block_rows, dtype=jnp.int32)) // SPAN
        visible = key_span[None, :] <= query_span[:, None]
        first_map = one_map(query_block[..., :QK], key_all[..., :QK], value_all, visible)
        second_map = one_map(query_block[..., QK:], key_all[..., QK:], value_all, visible)
        mixture = first_map - diff_scale[:, None, None] * second_map
        scale_back = lax.rsqrt(lax.optimization_barrier(jnp.mean(mixture * mixture, axis=-1, keepdims=True)) + NORM_EPS)
        attended = (mixture * scale_back * head_gain * HEAD_KEEP).astype(jnp.bfloat16)
        return jnp.transpose(attended, (1, 0, 2)).reshape(block_rows, HEADS * V)
    attended = lax.map(attend, jnp.arange(TOKENS // block_rows, dtype=jnp.int32)).reshape(TOKENS, HEADS * V)
    projected = jnp.dot(attended, out_weight, preferred_element_type=jnp.float32)
    after_mixer = (residual.astype(jnp.float32) + projected).astype(jnp.bfloat16)
    mixer_float = after_mixer.astype(jnp.float32)
    square_total = lax.optimization_barrier(jnp.sum(mixer_float * mixer_float, axis=-1, keepdims=True))
    normed = (mixer_float * lax.rsqrt(square_total / D + NORM_EPS) * norm_gain).astype(jnp.bfloat16)
    chosen = expert_ids.reshape(N_SP, TOK_DEV * TOP)
    onehot = (chosen[..., None] == jnp.arange(EXPERTS, dtype=jnp.int32)).astype(jnp.int32)
    rank_in = (lax.optimization_barrier(jnp.sum(jnp.cumsum(onehot, axis=1).astype(jnp.int32) * onehot, axis=-1)) - 1).astype(jnp.int32)
    source = jnp.arange(N_SP, dtype=jnp.int32)[:, None]
    per_expert = N_SP * CAP
    slot_index = (chosen * per_expert + source * CAP + rank_in).reshape(TOKENS * TOP).astype(jnp.int32)
    token_of = jnp.arange(TOKENS * TOP, dtype=jnp.int32) // TOP
    owner_row = jnp.full((EXPERTS * per_expert,), TOKENS, jnp.int32).at[slot_index].set(token_of)
    padded = jnp.concatenate([normed, jnp.zeros((1, D), jnp.bfloat16)], axis=0)

    def run_expert(expert):
        rows_in = padded[lax.dynamic_slice_in_dim(owner_row, (expert * per_expert).astype(jnp.int32), per_expert, 0)]
        pre_gate = jnp.dot(rows_in, gate_weight[expert], preferred_element_type=jnp.float32)
        pre_up = jnp.dot(rows_in, up_weight[expert], preferred_element_type=jnp.float32)
        capped = jnp.minimum(pre_gate, CLAMP_LIMIT)
        linear = jnp.clip(pre_up, -CLAMP_LIMIT, CLAMP_LIMIT)
        hidden = (capped * jax.nn.sigmoid(SWISH_ALPHA * capped) * (linear + 1.0)).astype(jnp.bfloat16)
        return jnp.dot(hidden, down_weight[expert], preferred_element_type=jnp.float32).astype(jnp.bfloat16)
    expert_out = lax.map(run_expert, jnp.arange(EXPERTS, dtype=jnp.int32)).reshape(EXPERTS * per_expert, D)
    picked = expert_out[slot_index].astype(jnp.float32).reshape(TOKENS, TOP, D)
    weights = jax.nn.softmax(route_logit.astype(jnp.float32), axis=-1)
    routed = lax.optimization_barrier(jnp.sum(picked * weights[..., None], axis=1))
    return (mixer_float + routed).astype(jnp.bfloat16)
```

```python
import functools

import jax
import jax.numpy as jnp
from jax import lax
from jax.experimental import pallas as pl
from jax.experimental.pallas import tpu as pltpu
from jax.sharding import PartitionSpec as P

QK = 64
SPAN = 64
PAIR = 2

NORM_EPS = 1e-05
CLAMP_LIMIT = 7.0
SWISH_ALPHA = 1.702
HEAD_KEEP = 0.8
NEG_FILL = -1e30

BF = jnp.bfloat16
F32 = jnp.float32


VM = pl.BlockSpec(memory_space=pltpu.VMEM)
SM = pl.BlockSpec(memory_space=pltpu.SMEM)


def dot(a, b, dims=((1,), (0,))):
    return lax.dot_general(a, b, (dims, ((), ())), preferred_element_type=F32)


def swap(value, axis, mask, size):
    if mask == 0:
        return value
    return lax.ppermute(value, axis, [(i, i ^ mask) for i in range(size)])


def call(body, out_shape, in_specs, scratch=(), flops=0, nbytes=0, name=None):
    out_specs = jax.tree.map(lambda _: VM, out_shape)
    return pl.pallas_call(
        body,
        out_shape=out_shape,
        in_specs=in_specs,
        out_specs=out_specs,
        scratch_shapes=list(scratch),
        cost_estimate=pl.CostEstimate(flops=flops, bytes_accessed=nbytes, transcendentals=0),
        name=name,
    )


def pack_body(meta, q, k, v, *outs):
    heads = q.shape[1]
    for h in range(heads):
        parts = [r[:, h, :] for r in (q, k, v)]
        for m in range(heads):
            @pl.when(meta[0] == (h ^ m))
            def _():
                for i, part in enumerate(parts):
                    outs[m][:, i * 128:(i + 1) * 128] = part


def attention_body(groups, members, tok, meta, scale, gain, *refs):
    own = refs[:groups]
    other = refs[groups:groups * members]
    outs = refs[groups * members:groups * members + groups]
    q_all, k_all, v_all = refs[groups * members + groups:]
    g, x = meta[0], meta[1]
    width = gain.shape[1]

    def put(dst, block, value):
        dst[pl.ds(pl.multiple_of(block * tok, tok), tok), :] = value

    for m in range(groups):
        row = jnp.bitwise_xor(g, m)
        put(q_all, row, own[m][:, :width])
        put(k_all, row * members + x, own[m][:, width:2 * width])
        put(v_all, row * members + x, own[m][:, 2 * width:])
        for j in range(1, members):
            piece = other[m * (members - 1) + j - 1]
            column = row * members + jnp.bitwise_xor(x, j)
            put(k_all, column, piece[:, :width])
            put(v_all, column, piece[:, width:])
    first_half = lax.broadcasted_iota(jnp.int32, (tok, width), 1) < QK
    local = members * tok
    query_span = x * (tok // SPAN) + lax.broadcasted_iota(jnp.int32, (2, tok, local), 1) // SPAN
    key_span = lax.broadcasted_iota(jnp.int32, (2, tok, local), 2) // SPAN
    visible = (key_span <= query_span).reshape(2 * tok, local)
    for b in range(groups):
        q = q_all[b * tok:(b + 1) * tok, :] * jnp.asarray(QK ** -0.5, BF)
        zero = jnp.zeros_like(q)
        both = jnp.concatenate([jnp.where(first_half, q, zero), jnp.where(first_half, zero, q)], axis=0)
        near = dot(both, k_all[b * local:(b + 1) * local, :], ((1,), (1,)))
        near = jnp.where(visible, near, NEG_FILL)
        peak = jnp.max(near, axis=1, keepdims=True)
        if b:
            far = dot(both, k_all[:b * local, :], ((1,), (1,)))
            peak = jnp.maximum(peak, jnp.max(far, axis=1, keepdims=True))
        near = jnp.exp(near - peak)
        total = jnp.sum(near, axis=1, keepdims=True)
        accum = dot(near.astype(BF), v_all[b * local:(b + 1) * local, :])
        if b:
            far = jnp.exp(far - peak)
            total = total + jnp.sum(far, axis=1, keepdims=True)
            accum = accum + dot(far.astype(BF), v_all[:b * local, :])
        value = accum / total
        mixture = value[:tok] - scale[g] * value[tok:]
        back = lax.rsqrt(jnp.mean(mixture * mixture, axis=1, keepdims=True) + NORM_EPS)
        attended = (mixture * back * gain[...] * HEAD_KEEP).astype(BF)
        for m in range(groups):
            @pl.when(g == (b ^ m))
            def _():
                outs[m][...] = attended


def route_body(zones, experts, cap, meta, ids, ids_t, logit, send, take0, take1, weight):
    tok = ids.shape[0]
    z, x = meta[2], meta[3]
    lanes = max(128, experts)

    def slot_of(expert, rank):
        zone = jnp.bitwise_xor(lax.shift_right_logical(expert, 1), z)
        side = jnp.bitwise_xor(jnp.bitwise_and(expert, 1), x)
        return (side * zones + zone) * cap + rank

    cols = lax.broadcasted_iota(jnp.int32, (tok, lanes), 1)
    first, second = ids[:, 0:1], ids[:, 1:2]
    hot0, hot1 = (cols == first).astype(F32), (cols == second).astype(F32)
    row = lax.broadcasted_iota(jnp.int32, (tok, tok), 0)
    col = lax.broadcasted_iota(jnp.int32, (tok, tok), 1)
    count = dot((col < row).astype(BF), (hot0 + hot1).astype(BF))
    slots = lax.broadcasted_iota(jnp.int32, (tok, take0.shape[1]), 1)
    for expert, hot, out in ((first, hot0, take0), (second, hot1, take1)):
        rank = jnp.sum(count * hot, axis=1, keepdims=True).astype(jnp.int32)
        out[...] = (slots == slot_of(expert, rank)).astype(BF)
    rows = lax.broadcasted_iota(jnp.int32, (lanes, tok), 0)
    first, second = ids_t[0:1, :], ids_t[1:2, :]
    hot0, hot1 = (rows == first).astype(F32), (rows == second).astype(F32)
    count = dot((hot0 + hot1).astype(BF), (row < col).astype(BF))
    slots = lax.broadcasted_iota(jnp.int32, (send.shape[0], tok), 0)
    pick = None
    for expert, hot in ((first, hot0), (second, hot1)):
        rank = jnp.sum(count * hot, axis=0, keepdims=True).astype(jnp.int32)
        mine = slots == slot_of(expert, rank)
        pick = mine if pick is None else jnp.logical_or(pick, mine)
    send[...] = pick.astype(BF)
    peak = jnp.max(logit[...], axis=1, keepdims=True)
    raised = jnp.exp(logit[...] - peak)
    weight[...] = raised / jnp.sum(raised, axis=1, keepdims=True)


def project_body(groups, heads, meta, residual, weight, send, *refs):
    slices, (mixer, kept, sent) = refs[:-3], refs[-3:]
    g, tp = meta[0], meta[4]
    width = weight.shape[0] // (heads * len(slices))
    total = residual[...].astype(F32)
    for m2, piece in enumerate(slices):
        for m in range(groups):
            head = jnp.bitwise_xor(tp, m2) * heads + jnp.bitwise_xor(g, m)
            start = pl.multiple_of(head * width, width)
            total = total + dot(piece[:, m * width:(m + 1) * width], weight[pl.ds(start, width), :])
    mixed = total.astype(BF)
    mixer[...] = mixed
    half = kept.shape[0]
    kept[...] = dot(send[:half, :], mixed).astype(BF)
    sent[...] = dot(send[half:, :], mixed).astype(BF)


def expert_in_body(parts, meta, gain, *refs):
    slices = refs[:parts]
    gate, up, hidden, normed = refs[parts:]
    tp = meta[4]
    width = slices[0].shape[1]

    def offset(m):
        return pl.multiple_of(jnp.bitwise_xor(tp, m) * width, width)

    @pl.when(pl.program_id(0) == 0)
    def _():
        values = [s[...].astype(F32) for s in slices]
        square = sum(jnp.sum(v * v, axis=1, keepdims=True) for v in values)
        back = lax.rsqrt(square / (width * parts) + NORM_EPS)
        for m, v in enumerate(values):
            normed[:, m * width:(m + 1) * width] = (v * back * gain[:, pl.ds(offset(m), width)]).astype(BF)

    pre_gate = pre_up = None
    for m in range(parts):
        rows = normed[:, m * width:(m + 1) * width]
        add_gate = dot(rows, gate[0, pl.ds(offset(m), width), :])
        add_up = dot(rows, up[0, pl.ds(offset(m), width), :])
        pre_gate = add_gate if m == 0 else pre_gate + add_gate
        pre_up = add_up if m == 0 else pre_up + add_up
    capped = jnp.minimum(pre_gate, CLAMP_LIMIT)
    linear = jnp.clip(pre_up, -CLAMP_LIMIT, CLAMP_LIMIT)
    hidden[...] = (capped * jax.nn.sigmoid(SWISH_ALPHA * capped) * (linear + 1.0)).astype(BF)


def expert_out_body(chips, meta, own, other, *refs):
    weights, outs = refs[:chips], refs[chips:]
    core = meta[6]
    half = own.shape[1]
    mine = pl.multiple_of(core * half, half)
    theirs = pl.multiple_of((1 - core) * half, half)
    for w, out in zip(weights, outs):
        w = w.at[0] if len(w.shape) == 3 else w
        total = dot(own[...], w[pl.ds(mine, half), :]) + dot(other[...], w[pl.ds(theirs, half), :])
        out[...] = total.astype(out.dtype)


def final_body(count, mixer, take0, take1, weight, *refs):
    pieces, out, rows = refs[:count], refs[count], refs[count + 1]
    at = 0
    for piece in pieces:
        rows[at:at + piece.shape[0], :] = piece[...]
        at += piece.shape[0]
    routed = weight[:, 0:1] * dot(take0[...], rows[...]) + weight[:, 1:2] * dot(take1[...], rows[...])
    out[...] = (mixer[...].astype(F32) + routed).astype(BF)


def local(
    residual,
    queries,
    key_rows,
    value_rows,
    diff_scale,
    head_gain,
    out_weight,
    norm_gain,
    gate_weight,
    up_weight,
    down_weight,
    expert_ids,
    route_logit,
):
    tok, heads, width = queries.shape
    n_sp, n_tp = lax.axis_size("sp"), lax.axis_size("tp")
    top = expert_ids.shape[1]
    groups, members = heads, n_sp // heads
    zones, chips = n_sp // PAIR, n_tp // PAIR
    cap = 2 * tok * top // n_sp
    column = residual.shape[1]
    features = column * n_tp
    units = gate_weight.shape[2]
    rows = PAIR * cap
    sp, tp = lax.axis_index("sp"), lax.axis_index("tp")
    meta = jnp.stack([sp // members, sp % members, sp // PAIR, sp % PAIR, tp, tp // PAIR, tp % PAIR])
    meta = meta.astype(jnp.int32)

    def shape(*dims, dtype=BF):
        return jax.ShapeDtypeStruct(dims, dtype)

    packed = call(
        pack_body, [shape(tok, 3 * width)] * groups, [SM, VM, VM, VM], name="pack",
    )(meta, queries, key_rows, value_rows)
    order = sorted(range(groups), reverse=True)
    own = [None] * groups
    other = [None] * groups
    for m in order:
        own[m] = swap(packed[m], "sp", m * members, n_sp)
    for m in order:
        other[m] = [swap(own[m][:, width:], "sp", j, n_sp) for j in range(1, members)]
    others = [piece for m in range(groups) for piece in other[m]]

    chip = tp // PAIR
    share = units * PAIR
    down = [down_weight]
    for yy in range(1, chips):
        start = jnp.bitwise_xor(chip, yy) * share
        part = lax.dynamic_slice_in_dim(down_weight[0], start, share, 0)
        down.append(swap(part, "tp", yy * PAIR, n_tp))

    send, take0, take1, weights = call(
        functools.partial(route_body, zones, n_sp, cap),
        [shape(n_sp * cap, tok), shape(tok, n_sp * cap), shape(tok, n_sp * cap), shape(tok, top, dtype=F32)],
        [SM, VM, VM, VM],
        name="route",
    )(meta, expert_ids, expert_ids.T, route_logit)

    pairs = 2 * tok * tok * members * sum(range(1, groups + 1))
    attended = call(
        functools.partial(attention_body, groups, members, tok),
        [shape(tok, width)] * groups,
        [SM, SM, VM] + [VM] * (groups * members),
        scratch=[
            pltpu.VMEM((groups * tok, width), BF),
            pltpu.VMEM((n_sp * tok, width), BF),
            pltpu.VMEM((n_sp * tok, width), BF),
        ],
        flops=4 * pairs * width * 4,
        name="attention",
    )(meta, diff_scale, head_gain.reshape(1, -1), *own, *others)
    back = [swap(attended[m], "sp", m * members, n_sp) for m in range(groups)]
    block = jnp.concatenate(back, axis=1)

    def gather_tp(value):
        columns = [swap(value, "tp", yy * PAIR, n_tp) for yy in range(chips)]
        return [columns[m // PAIR] if m % PAIR == 0 else swap(columns[m // PAIR], "tp", 1, n_tp)
                for m in range(n_tp)]

    mixer, kept, sent = call(
        functools.partial(project_body, groups, heads),
        [shape(tok, column), shape(zones * cap, column), shape(zones * cap, column)],
        [SM] + [VM] * (3 + n_tp),
        flops=2 * tok * features * column * 4,
        name="project",
    )(meta, residual, out_weight, send, *gather_tp(block))

    gain = norm_gain.reshape(1, -1)
    tile = min(units, 256)
    returned = [None] * zones
    for m in sorted(range(zones), reverse=True):
        crossed = swap(sent[m * cap:(m + 1) * cap], "sp", 1, n_sp)
        piece = jnp.concatenate([kept[m * cap:(m + 1) * cap], crossed], axis=0)
        piece = swap(piece, "sp", m * PAIR, n_sp)
        hidden = pl.pallas_call(
            functools.partial(expert_in_body, n_tp),
            out_shape=shape(rows, units),
            grid_spec=pltpu.PrefetchScalarGridSpec(
                num_scalar_prefetch=1,
                grid=(units // tile,),
                in_specs=[pl.BlockSpec((1, features), lambda i, s: (0, 0))]
                + [pl.BlockSpec((rows, column), lambda i, s: (0, 0))] * n_tp
                + [pl.BlockSpec((1, features, tile), lambda i, s: (0, 0, i))] * 2,
                out_specs=pl.BlockSpec((rows, tile), lambda i, s: (0, i)),
                scratch_shapes=[pltpu.VMEM((rows, features), BF)],
            ),
            cost_estimate=pl.CostEstimate(
                flops=4 * rows * features * units * 2, bytes_accessed=4 * features * units, transcendentals=0
            ),
            name="expert_in",
        )(meta, gain, *gather_tp(piece), gate_weight, up_weight)
        beside = swap(hidden, "tp", 1, n_tp)
        partial = pl.pallas_call(
            functools.partial(expert_out_body, chips),
            out_shape=[shape(rows, column, dtype=F32 if yy == 0 else BF) for yy in range(chips)],
            grid_spec=pltpu.PrefetchScalarGridSpec(
                num_scalar_prefetch=1,
                grid=(1,),
                in_specs=[pl.BlockSpec((rows, units), lambda i, s: (0, 0))] * 2
                + [pl.BlockSpec((1, share, column), lambda i, s: (0, s[5], 0))]
                + [pl.BlockSpec((share, column), lambda i, s: (0, 0))] * (chips - 1),
                out_specs=[pl.BlockSpec((rows, column), lambda i, s: (0, 0))] * chips,
            ),
            cost_estimate=pl.CostEstimate(
                flops=2 * rows * share * column * chips * 2, bytes_accessed=2 * share * column * chips, transcendentals=0
            ),
            name="expert_out",
        )(meta, hidden, beside, *down)
        total = partial[0]
        for yy in range(1, chips):
            total = total + swap(partial[yy], "tp", yy * PAIR, n_tp).astype(F32)
        result = swap(total.astype(BF), "sp", m * PAIR, n_sp)
        returned[m] = (result[:cap], swap(result[cap:], "sp", 1, n_sp))

    pieces = [r[0] for r in returned] + [r[1] for r in returned]
    return call(
        functools.partial(final_body, len(pieces)),
        shape(tok, column),
        [VM] * (4 + len(pieces)),
        scratch=[pltpu.VMEM((n_sp * cap, column), BF)],
        flops=4 * tok * n_sp * cap * column,
        name="final",
    )(mixer, take0, take1, weights, *pieces)


def solution(mesh):
    return jax.shard_map(
        local,
        mesh=mesh,
        in_specs=(
            P("sp", "tp"),
            P("sp", "tp", None),
            P("sp", "tp", None),
            P("sp", "tp", None),
            P("tp"),
            P(),
            P(None, "tp"),
            P(),
            P("sp", None, "tp"),
            P("sp", None, "tp"),
            P("sp", None, "tp"),
            P("sp", None),
            P("sp", None),
        ),
        out_specs=P("sp", "tp"),
        check_vma=False,
    )
```
